32 devices in a mesh: sp: 4 (over y, x), tp: 8 (over z, core).
Axes of the slice: x: 2, y: 2, z: 4, core: 2. Of those that a mesh axis runs over, the one named last changes fastest.
Arguments:
- queries: bfloat16 [1536, 2048], P('sp', 'tp'), may hold values from -6 to 6
- cell_key_rows: bfloat16 [1536, 2048], P('sp', 'tp'), may hold values from -6 to 6
- cell_value_rows: bfloat16 [1536, 2048], P('sp', 'tp'), may hold values from -6 to 6
- output_gate_logits: bfloat16 [1536, 2048], P('sp', 'tp'), may hold values from -6 to 6
- input_gate_logs: float32 [16, 1536], P('tp', 'sp'), may hold values from -5 to 250
- forget_gate_logits: float32 [16, 1536], P('tp', 'sp'), may hold values from 1 to 13
- extra_log_forget: float32 [16, 1536], P('tp', 'sp'), may hold values from -0.7 to 0
- head_norm_gain: float32 [2048], P('tp'), may hold values from 0.1 to 1.9
- cell_output_matrix: bfloat16 [2048, 4096], P('tp'), may hold values from -0.125 to 0.125
- residual: bfloat16 [1536, 4096], P('sp'), may hold values from -6 to 6
- expert_norm_gain: float32 [4096], replicated, may hold values from 0.1 to 1.9
- routes: int32 [1536, 2], P('sp'), may hold values from 0 to 3, all different within a row; in each aligned block of 48 rows (0 to 47, 48 to 95, ...) at most 48 rows name the same one
- token_expert_weights: float32 [1536, 2], P('sp'), may hold values from 0.2 to 1
- expert_gate_matrix: bfloat16 [4, 4096, 2048], P('sp', None, 'tp'), may hold values from -0.09375 to 0.09375
- expert_up_matrix: bfloat16 [4, 4096, 2048], P('sp', None, 'tp'), may hold values from -0.09375 to 0.09375
- expert_down_matrix: bfloat16 [4, 2048, 4096], P('sp', 'tp'), may hold values from -0.125 to 0.125
Outputs:
- layer_out: bfloat16 [1536, 4096], P(('sp', 'tp'))
The draws below stay inside these ranges and needn't reach their ends.
Inputs may be any that keep to these rules, and one draw needn't show every extreme that they name: `routes`: each row names 2 different experts. In the rows of one device (aligned blocks of 48 rows) no expert is named more than 48 times, and in some blocks one expert is named exactly 48 times.
All inputs are finite; a program needn't handle non-finite values.
Results may differ from the reference program's by a relative error of at most 0.019.
Values may be sent and summed in bfloat16 or wider, within the bound.
No kernel may reach another device: no remote copies, remote signals or barrier semaphores. Data moves between devices by JAX's collectives and lax.ppermute only.
A program may use at most 128 MiB of HBM per device.

```python
import math
import jax
import jax.numpy as jnp
import numpy as np
from jax import lax

D = 4096
HEADS = 16
HEAD_DIM = 128
MIX = 2048
FF = 2048
EXPERTS = 4
TOPK = 2
S_DEV = 384
SEQ = 1536
TOK_DEV = 48
CAP = 48
BLOCK = 128
N_TP = 8


def draw_forget_gate_logits(key, part):
    slow_key, shift_key, noise_key = jax.random.split(jax.random.fold_in(key, 11), 3)
    pick = jax.random.uniform(slow_key, (HEADS, 1))
    slow = pick < 0.5
    noise = 0.5 * jnp.clip(jax.random.normal(noise_key, (HEADS, SEQ)), -3.0, 3.0)
    base = jnp.where(slow, jnp.log(2.0 * SEQ), jnp.log(40.0))
    shifts = jax.random.uniform(shift_key, (HEADS, SEQ // S_DEV), minval=-1.0, maxval=1.0)
    return (base + jnp.repeat(shifts, S_DEV, axis=1) + noise).astype(jnp.float32)


def draw_input_gate_logs(key, part):
    base_key = jax.random.fold_in(jax.random.fold_in(key, 13), 0)
    values = jnp.clip(jax.random.normal(base_key, (HEADS, SEQ)), -5.0, 5.0)
    return values.astype(jnp.float32)


def draw_extra_log_forget(key, part):
    place_key, size_key = jax.random.split(jax.random.fold_in(key, 17), 2)
    planted = jax.random.uniform(place_key, (HEADS, SEQ)) < 3.0 / SEQ
    sizes = jnp.log(jax.random.uniform(size_key, (HEADS, SEQ), minval=0.5, maxval=0.8))
    return jnp.where(planted, sizes, 0.0).astype(jnp.float32)


def block_levels(stream_key, shape, shards, least, top_value):
    loudness = 1.0
    for position, shards_of in shards:
        steps = jax.random.uniform(jax.random.fold_in(jax.random.fold_in(stream_key, 6), position), (shards_of,), jnp.float32, least / len(shards), top_value / len(shards))
        loudness = loudness * jnp.repeat(jnp.exp(steps), shape[position] // shards_of).reshape((-1,) + (1,) * (len(shape) - 1 - position))
    return loudness


def assign_block(rng, own, number, rows, amount, top, most, lean):
    order = jax.random.permutation(rng, amount)
    heavy_load, usual = load_shares(amount, rows * top, most, lean, True), load_shares(amount, rows * top, most, lean, False)
    places = jnp.arange(amount)

    def named(tallies, rotation):
        used = int((tallies > 0).sum())
        fixed = max(1, used // 4)
        passed = fixed + (places - fixed + rotation * (used - fixed)) % max(1, amount - fixed)
        return jnp.zeros((amount,), jnp.int32).at[order[jnp.where(places < fixed, places, passed)]].set(jnp.asarray(tallies, jnp.int32))

    tallies = jnp.where(number % 4 == 0, named(heavy_load, number // 4), named(usual, number - number // 4 - 1))
    mixed = jax.random.permutation(jax.random.fold_in(own, 3), amount)
    giver, sink = mixed[0:amount // 2 * 2:2], mixed[1:amount // 2 * 2:2]
    slack = jnp.minimum(tallies[giver] - 1, most - tallies[sink]) // 2
    slack = jnp.where((giver == order[0]) | (sink == order[0]) | (tallies[sink] == 0), 0, jnp.maximum(slack, 0))
    passed = jax.random.randint(jax.random.fold_in(own, 4), (amount // 2,), 0, 1 << 20) % (slack + 1)
    tallies = tallies.at[giver].add(-passed).at[sink].add(passed)
    items = jnp.searchsorted(jnp.cumsum(tallies), jnp.arange(rows * top), side="right").astype(jnp.int32)
    listing = items.reshape(top, rows).T
    listing = listing[jax.random.permutation(jax.random.fold_in(own, 1), rows)]
    rotation = jax.random.randint(jax.random.fold_in(own, 2), (rows, 1), 0, top)
    return jnp.take_along_axis(listing, (jnp.arange(top)[None, :] + rotation) % top, axis=1)


def load_shares(number_of, total, most, slope, full):
    weights = [(1 << 20) // math.isqrt(rank ** slope) + 1 for rank in range(1, number_of + 1)]
    largest = most if full else min(most, max(-(-total // number_of), total * weights[0] // sum(weights)))
    least = 1 if total - largest >= number_of - 1 else 0
    given, rest = [largest] + [least] * (number_of - 1), total - largest - least * (number_of - 1)
    while rest > 0:
        movable = [i for i in range(1, number_of) if given[i] < largest] or [i for i in range(1, number_of) if given[i] < most]
        mass, left = sum([weights[i] for i in movable]), rest
        for i in movable:
            more = min(most - given[i], max(1, left * weights[i] // mass), rest)
            given[i] = given[i] + more
            rest = rest - more
    return np.array(given)


def centred(stream_key, extent, scale, reach, shards=(), held_as=jnp.bfloat16):
    loudness = block_levels(stream_key, extent, shards, -0.22, 0.18) if shards else 1.0
    drawn = jax.random.normal(stream_key, extent, jnp.float32) * scale * loudness
    return jnp.minimum(jnp.maximum(drawn, -reach), reach).astype(held_as)


def setup_inputs(seed: int = 0) -> dict:
    key_list = jax.random.split(jax.random.key(seed), 17)
    queries = centred(key_list[0], (SEQ, MIX), 1.0, 6.0, ((0, 4), (1, 8)))
    cell_key_rows = centred(key_list[1], (SEQ, MIX), 1.0, 6.0, ((0, 4), (1, 8)))
    cell_value_rows = centred(key_list[2], (SEQ, MIX), 1.0, 6.0, ((0, 4), (1, 8)))
    output_gate_logits = centred(key_list[3], (SEQ, MIX), 1.0, 6.0, ((0, 4), (1, 8)))
    input_gate_logs = draw_input_gate_logs(jax.random.fold_in(key_list[16], 71), 0)
    forget_gate_logits = draw_forget_gate_logits(jax.random.fold_in(key_list[16], 71), 0)
    extra_log_forget = draw_extra_log_forget(jax.random.fold_in(key_list[16], 71), 0)
    head_norm_gain = jnp.clip(1.0 + 0.18 * jax.random.normal(key_list[7], (MIX,), jnp.float32), 0.1, 1.9)
    cell_output_matrix = centred(key_list[8], (MIX, D), MIX ** -0.5, 0.125, ((0, 8),))
    residual = centred(key_list[9], (SEQ, D), 1.0, 6.0, ((0, 4),))
    expert_norm_gain = jnp.clip(1.0 + 0.18 * jax.random.normal(key_list[10], (D,), jnp.float32), 0.1, 1.9)
    routes_keys = jax.random.split(jax.random.fold_in(key_list[11], 1), SEQ // TOK_DEV)
    routes_turns = jax.random.permutation(jax.random.fold_in(key_list[11], 3), SEQ // TOK_DEV)
    routes = jax.vmap(lambda own, number: assign_block(jax.random.fold_in(key_list[11], 2), own, number, TOK_DEV, EXPERTS, TOPK, CAP, 2))(routes_keys, routes_turns).reshape((SEQ, TOPK))
    token_expert_weights = jnp.clip(jnp.exp(math.log(1.0) - 1.609438 * jax.random.uniform(key_list[12], (SEQ, TOPK), jnp.float32) ** block_levels(key_list[12], (SEQ, TOPK), ((0, 4),), -0.2, 0.2)), 0.2, 1.0)
    expert_gate_matrix = centred(key_list[13], (EXPERTS, D, FF), D ** -0.5, 0.09375, ((0, 4), (2, 8)))
    expert_up_matrix = centred(key_list[14], (EXPERTS, D, FF), D ** -0.5, 0.09375, ((0, 4), (2, 8)))
    expert_down_matrix = centred(key_list[15], (EXPERTS, FF, D), FF ** -0.5, 0.125, ((0, 4), (1, 8)))
    return dict(queries=queries, cell_key_rows=cell_key_rows, cell_value_rows=cell_value_rows, output_gate_logits=output_gate_logits, input_gate_logs=input_gate_logs, forget_gate_logits=forget_gate_logits, extra_log_forget=extra_log_forget, head_norm_gain=head_norm_gain, cell_output_matrix=cell_output_matrix, residual=residual, expert_norm_gain=expert_norm_gain, routes=routes, token_expert_weights=token_expert_weights, expert_gate_matrix=expert_gate_matrix, expert_up_matrix=expert_up_matrix, expert_down_matrix=expert_down_matrix)


floor_neg = -1e+30
norm_eps = 1e-06
row_group = 128

def block_cells(query_f, key_f, value_f, input_f, forget_log_values, start_cell, start_stab):
    heads, length, width = query_f.shape
    count = length // BLOCK
    highest = lax.Precision.HIGHEST

    def split(array):
        return jnp.moveaxis(array.reshape((heads, count, BLOCK) + array.shape[2:]), 1, 0)
    causal = jnp.tril(jnp.ones((BLOCK, BLOCK), dtype=bool))

    def advance(carry, block):
        cell, stab = carry
        qblock, kblock, vblock, iblock, fblock = block
        cumul = jnp.cumsum(fblock, axis=-1)
        total = cumul[:, -1]
        log_inner = jnp.where(causal[None], cumul[:, :, None] - cumul[:, None, :] + iblock[:, None, :], floor_neg)
        carried = cumul + stab[:, None]
        stab_row = jnp.maximum(carried, lax.optimization_barrier(jnp.max(log_inner, axis=-1)))
        scores = jnp.einsum('hld,hsd->hls', qblock, kblock, precision=highest) * jnp.exp(log_inner - stab_row[..., None])
        numer = jnp.einsum('hls,hsd->hld', scores, vblock, precision=highest) + jnp.exp(carried - stab_row)[..., None] * jnp.einsum('hld,hde->hle', qblock, cell, precision=highest)
        log_write = total[:, None] - cumul + iblock
        stab_next = jnp.maximum(total + stab, lax.optimization_barrier(jnp.max(log_write, axis=-1)))
        weights = jnp.exp(log_write - stab_next[:, None])
        cell_next = jnp.exp(total + stab - stab_next)[:, None, None] * cell + jnp.einsum('hsd,hse->hde', kblock * weights[..., None], vblock, precision=highest)
        return ((cell_next, stab_next), (numer, stab_row))
    inputs = tuple((split(array) for array in (query_f, key_f, value_f, input_f, forget_log_values)))
    unused, (numer, stab_rows) = lax.scan(advance, (start_cell, start_stab), inputs)
    numer = jnp.moveaxis(numer, 0, 1).reshape(heads, length, width)
    stab_rows = jnp.moveaxis(stab_rows, 0, 1).reshape(heads, length)
    return (numer, stab_rows)

def rms_scale(rows, gain):
    values = rows.astype(jnp.float32)
    return (values * lax.rsqrt(lax.optimization_barrier(jnp.mean(values * values, axis=-1, keepdims=True)) + norm_eps) * gain).astype(jnp.bfloat16)

def expert_outputs(moe_in, routes, expert_gate_matrix, expert_up_matrix, expert_down_matrix):
    count = SEQ * TOPK
    expert = routes.reshape(-1).astype(jnp.int32)
    owner = jnp.arange(count, dtype=jnp.int32) // TOPK
    order = jnp.argsort(expert, stable=True).astype(jnp.int32)
    sorted_expert = expert[order]
    loads = lax.optimization_barrier(jnp.sum((expert[:, None] == jnp.arange(EXPERTS, dtype=jnp.int32)[None, :]).astype(jnp.int32), axis=0))
    starts = (jnp.cumsum(loads) - loads).astype(jnp.int32)
    padded = ((loads + row_group - 1) // row_group * row_group).astype(jnp.int32)
    ends = jnp.cumsum(padded).astype(jnp.int32)
    padded_starts = ends - padded
    dest = (padded_starts[sorted_expert] + jnp.arange(count, dtype=jnp.int32) - starts[sorted_expert]).astype(jnp.int32)
    room = (count + row_group - 1) // row_group * row_group + EXPERTS * row_group
    blocks = room // row_group
    row_owner = jnp.full((room,), SEQ, jnp.int32).at[dest].set(owner[order])
    block_first = jnp.arange(blocks, dtype=jnp.int32) * row_group
    block_expert = jnp.minimum(lax.optimization_barrier(jnp.sum((block_first[:, None] >= ends[None, :]).astype(jnp.int32), axis=1)), EXPERTS - 1).astype(jnp.int32)
    padded_in = jnp.concatenate([moe_in, jnp.zeros((1, D), moe_in.dtype)], axis=0)
    block_rows = padded_in[row_owner].reshape(blocks, row_group, D)
    width = FF // N_TP

    def one_block(args):
        rows, which = args
        gate = jnp.dot(rows, expert_gate_matrix[which], preferred_element_type=jnp.float32)
        upper = jnp.dot(rows, expert_up_matrix[which], preferred_element_type=jnp.float32)
        hidden = (jax.nn.silu(gate) * upper).astype(jnp.bfloat16)
        parts = jnp.einsum('rjf,jfd->rjd', hidden.reshape(row_group, N_TP, width).astype(jnp.float32), expert_down_matrix[which].reshape(N_TP, width, D).astype(jnp.float32))
        parts = lax.optimization_barrier(parts.astype(jnp.bfloat16)).astype(jnp.float32)
        return lax.optimization_barrier(jnp.sum(parts, axis=1)).astype(jnp.bfloat16)
    outputs = lax.map(one_block, (block_rows, block_expert)).reshape(room, D)
    place = jnp.zeros((count,), jnp.int32).at[order].set(dest)
    return outputs[place].reshape(SEQ, TOPK, D)

def reference(queries, cell_key_rows, cell_value_rows, output_gate_logits, input_gate_logs, forget_gate_logits, extra_log_forget, head_norm_gain, cell_output_matrix, residual, expert_norm_gain, routes, token_expert_weights, expert_gate_matrix, expert_up_matrix, expert_down_matrix):

    def heads_of(array):
        return jnp.transpose(array.astype(jnp.float32).reshape(SEQ, HEADS, HEAD_DIM), (1, 0, 2))
    query_f = heads_of(queries)
    key_f = heads_of(cell_key_rows) * HEAD_DIM ** (-0.5)
    value_f = heads_of(cell_value_rows)
    forget_log_values = jax.nn.log_sigmoid(forget_gate_logits) + extra_log_forget
    numer, stab_rows = block_cells(query_f, key_f, value_f, input_gate_logs, forget_log_values, jnp.zeros((HEADS, HEAD_DIM, HEAD_DIM), jnp.float32), jnp.zeros((HEADS,), jnp.float32))
    scaled = numer * lax.rsqrt(lax.optimization_barrier(jnp.mean(numer * numer, axis=2, keepdims=True)) + norm_eps) * head_norm_gain.reshape(HEADS, 1, HEAD_DIM)
    mixed = jnp.transpose(scaled, (1, 0, 2)).reshape(SEQ, MIX)
    cell_out = (jax.nn.sigmoid(output_gate_logits.astype(jnp.float32)) * mixed).astype(jnp.bfloat16)
    projected = jnp.dot(cell_out, cell_output_matrix, preferred_element_type=jnp.float32)
    after_mix = (residual.astype(jnp.float32) + projected).astype(jnp.bfloat16)
    moe_in = rms_scale(after_mix, expert_norm_gain)
    chosen = expert_outputs(moe_in, routes, expert_gate_matrix, expert_up_matrix, expert_down_matrix)
    moe = lax.optimization_barrier(jnp.sum(token_expert_weights[:, :, None] * chosen.astype(jnp.float32), axis=1))
    return (after_mix.astype(jnp.float32) + moe).astype(jnp.bfloat16)
```

```python
import jax
import jax.numpy as jnp
from jax import lax
from jax.sharding import PartitionSpec as P

HEAD_DIM = 128
BLOCK = 128


floor_neg = -1e30
norm_eps = 1e-06


def entering(x, axis, combine, identity):
    count, here = (lax.axis_size(axis), lax.axis_index(axis))
    everything = jax.tree.map(lambda part: lax.all_gather(part, axis), x)
    start = jax.tree.map(
        lambda part, zero: jnp.broadcast_to(jnp.asarray(zero, part.dtype), part.shape), x, identity
    )

    def lap(k, before):
        reached = k < here
        new = combine(before, jax.tree.map(lambda part: part[k], everything))
        return jax.tree.map(lambda a, b: jnp.where(reached, a, b), new, before)

    return lax.fori_loop(0, count, lap, start)


def block_cells(query_f, key_f, value_f, input_f, forget_log_values, start_cell, start_stab):
    heads, length, width = query_f.shape
    count = length // BLOCK
    highest = lax.Precision.HIGHEST

    def split(array):
        return jnp.moveaxis(array.reshape((heads, count, BLOCK) + array.shape[2:]), 1, 0)

    causal = jnp.tril(jnp.ones((BLOCK, BLOCK), dtype=bool))

    def advance(carry, block):
        cell, stab = carry
        qblock, kblock, vblock, iblock, fblock = block
        cumul = jnp.cumsum(fblock, axis=-1)
        total = cumul[:, -1]
        log_inner = jnp.where(
            causal[None], cumul[:, :, None] - cumul[:, None, :] + iblock[:, None, :], floor_neg
        )
        carried = cumul + stab[:, None]
        stab_row = jnp.maximum(carried, jnp.max(log_inner, axis=-1))
        scores = jnp.einsum("hld,hsd->hls", qblock, kblock, precision=highest) * jnp.exp(
            log_inner - stab_row[..., None]
        )
        numer = jnp.einsum("hls,hsd->hld", scores, vblock, precision=highest) + jnp.exp(
            carried - stab_row
        )[..., None] * jnp.einsum("hld,hde->hle", qblock, cell, precision=highest)
        log_write = total[:, None] - cumul + iblock
        stab_next = jnp.maximum(total + stab, jnp.max(log_write, axis=-1))
        weights = jnp.exp(log_write - stab_next[:, None])
        cell_next = jnp.exp(total + stab - stab_next)[:, None, None] * cell + jnp.einsum(
            "hsd,hse->hde", kblock * weights[..., None], vblock, precision=highest
        )
        return ((cell_next, stab_next), (numer, stab_row))

    inputs = tuple(
        (split(array) for array in (query_f, key_f, value_f, input_f, forget_log_values))
    )
    unused, (numer, stab_rows) = lax.scan(advance, (start_cell, start_stab), inputs)
    numer = jnp.moveaxis(numer, 0, 1).reshape(heads, length, width)
    stab_rows = jnp.moveaxis(stab_rows, 0, 1).reshape(heads, length)
    return (numer, stab_rows)


def combine_states(earlier, later):
    cell_early, stab_early, total_early = earlier
    cell_late, stab_late, total_late = later
    stab = jnp.maximum(total_late + stab_early, stab_late)
    cell = (
        jnp.exp(total_late + stab_early - stab)[:, None, None] * cell_early
        + jnp.exp(stab_late - stab)[:, None, None] * cell_late
    )
    return (cell, stab, total_early + total_late)


def rms_scale(rows, gain):
    values = rows.astype(jnp.float32)
    return (
        values * lax.rsqrt(jnp.mean(values * values, axis=-1, keepdims=True) + norm_eps) * gain
    ).astype(jnp.bfloat16)


def slot_tables(block_routes, experts, capacity):
    flat = block_routes.reshape(-1)
    count = flat.shape[0]
    topk = block_routes.shape[1]
    onehot = (flat[:, None] == jnp.arange(experts, dtype=jnp.int32)[None, :]).astype(jnp.int32)
    before = jnp.cumsum(onehot, axis=0) - onehot
    position = jnp.sum(before * onehot, axis=1)
    slot = flat * capacity + position
    match = slot[None, :] == jnp.arange(experts * capacity, dtype=jnp.int32)[:, None]
    owner = jnp.arange(count, dtype=jnp.int32)[None, :] // topk + 1
    source = jnp.sum(jnp.where(match, owner, 0), axis=1) - 1
    return (slot, source)


def fill_slots(rows, source):
    picked = rows[jnp.maximum(source, 0)]
    return jnp.where((source >= 0)[:, None], picked, jnp.zeros_like(picked))


def local(
    queries,
    cell_key_rows,
    cell_value_rows,
    output_gate_logits,
    input_gate_logs,
    forget_gate_logits,
    extra_log_forget,
    head_norm_gain,
    cell_output_matrix,
    residual,
    expert_norm_gain,
    routes,
    token_expert_weights,
    expert_gate_matrix,
    expert_up_matrix,
    expert_down_matrix,
):
    length = queries.shape[0]
    heads = queries.shape[1] // HEAD_DIM
    tp_count = lax.axis_size("tp")
    experts = lax.axis_size("sp")
    topk = routes.shape[1]
    tokens = length // tp_count
    capacity = max(2, 2 * tokens * topk // experts)
    highest = lax.Precision.HIGHEST
    tp_index = lax.axis_index("tp")

    def heads_of(array):
        return jnp.transpose(array.astype(jnp.float32).reshape(length, heads, HEAD_DIM), (1, 0, 2))

    query_f = heads_of(queries)
    key_f = heads_of(cell_key_rows) * HEAD_DIM ** (-0.5)
    value_f = heads_of(cell_value_rows)
    forget_log_values = jax.nn.log_sigmoid(forget_gate_logits) + extra_log_forget
    running = jnp.cumsum(forget_log_values, axis=1)
    total_dev = running[:, -1]
    log_write = input_gate_logs + total_dev[:, None] - running
    stab_dev = jnp.max(log_write, axis=1)
    cell_dev = jnp.einsum(
        "hsd,hse->hde",
        key_f * jnp.exp(log_write - stab_dev[:, None])[..., None],
        value_f,
        precision=highest,
    )
    identity = (
        jnp.zeros_like(cell_dev),
        jnp.full_like(stab_dev, floor_neg),
        jnp.zeros_like(total_dev),
    )
    prefix_cell, prefix_stab, prefix_total = entering(
        (cell_dev, stab_dev, total_dev), "sp", combine_states, identity
    )
    start_stab = jnp.maximum(prefix_stab, prefix_total)
    start_cell = jnp.exp(prefix_stab - start_stab)[:, None, None] * prefix_cell
    numer = block_cells(
        query_f, key_f, value_f, input_gate_logs, forget_log_values, start_cell, start_stab
    )[0]
    scaled = (
        numer
        * lax.rsqrt(jnp.mean(numer * numer, axis=2, keepdims=True) + norm_eps)
        * head_norm_gain.reshape(heads, 1, HEAD_DIM)
    )
    mixed = jnp.transpose(scaled, (1, 0, 2)).reshape(length, heads * HEAD_DIM)
    cell_out = (jax.nn.sigmoid(output_gate_logits.astype(jnp.float32)) * mixed).astype(jnp.bfloat16)
    gate_local = expert_gate_matrix[0]
    up_local = expert_up_matrix[0]
    down_local = expert_down_matrix[0]
    projected = lax.psum_scatter(
        jnp.dot(cell_out, cell_output_matrix, preferred_element_type=jnp.float32).astype(
            jnp.bfloat16
        ),
        "tp",
        scatter_dimension=0,
        tiled=True,
    ).astype(jnp.float32)
    own_residual = lax.dynamic_slice_in_dim(residual, tp_index * tokens, tokens, 0)
    after_mix = (own_residual.astype(jnp.float32) + projected).astype(jnp.bfloat16)
    own_routes = lax.dynamic_slice_in_dim(routes, tp_index * tokens, tokens, 0)
    slot, source = slot_tables(own_routes, experts, capacity)
    moe_in = rms_scale(after_mix, expert_norm_gain)
    sent = fill_slots(moe_in, source).reshape(experts, capacity, moe_in.shape[1])
    arrived = lax.all_to_all(sent, "sp", split_axis=0, concat_axis=0, tiled=True)
    piece = lax.all_gather(arrived, "tp", axis=0, tiled=True)
    gate = jnp.einsum("rcd,df->rcf", piece, gate_local, preferred_element_type=jnp.float32)
    upper = jnp.einsum("rcd,df->rcf", piece, up_local, preferred_element_type=jnp.float32)
    hidden = (jax.nn.silu(gate) * upper).astype(jnp.bfloat16)
    summed = lax.psum_scatter(
        jnp.einsum("rcf,fd->rcd", hidden, down_local, preferred_element_type=jnp.float32).astype(
            jnp.bfloat16
        ),
        "tp",
        scatter_dimension=0,
        tiled=True,
    )
    returned = lax.all_to_all(summed, "sp", split_axis=0, concat_axis=0, tiled=True)
    width = returned.shape[2]
    chosen = returned.reshape(experts * capacity, width)[slot].reshape(tokens, topk, width)
    own_weight = lax.dynamic_slice_in_dim(token_expert_weights, tp_index * tokens, tokens, 0)
    moe = jnp.sum(own_weight[:, :, None] * chosen.astype(jnp.float32), axis=1)
    return (after_mix.astype(jnp.float32) + moe).astype(jnp.bfloat16)


def exchange(kind, amount):
    sp_count, tp_count = lax.axis_size("sp"), lax.axis_size("tp")
    pairs = []
    for s in range(sp_count):
        for t in range(tp_count):
            if kind == "sp":
                to = (s ^ amount, t)
            elif kind == "core":
                to = (s, t ^ 1)
            else:
                to = (s, (t + 2 * amount) % tp_count)
            pairs.append((s * tp_count + t, to[0] * tp_count + to[1]))
    return pairs


def send(x, kind, amount=1):
    return lax.ppermute(x, ("sp", "tp"), exchange(kind, amount))


def relative(x, axis, start):
    size = x.shape[axis]
    return lax.dynamic_slice_in_dim(jnp.concatenate([x, x], axis), start, size, axis)


def dense_local(
    queries,
    cell_key_rows,
    cell_value_rows,
    output_gate_logits,
    input_gate_logs,
    forget_gate_logits,
    extra_log_forget,
    head_norm_gain,
    cell_output_matrix,
    residual,
    expert_norm_gain,
    routes,
    token_expert_weights,
    expert_gate_matrix,
    expert_up_matrix,
    expert_down_matrix,
):
    length = queries.shape[0]
    heads = queries.shape[1] // HEAD_DIM
    model = residual.shape[1]
    tp_count = lax.axis_size("tp")
    chips = tp_count // 2
    tokens = length // tp_count
    half = tokens // 2
    highest = lax.Precision.HIGHEST
    sp_index = lax.axis_index("sp")
    tp_index = lax.axis_index("tp")
    chip, core = tp_index // 2, tp_index % 2
    bf16 = jnp.bfloat16

    def heads_of(array):
        return jnp.transpose(array.astype(jnp.float32).reshape(length, heads, HEAD_DIM), (1, 0, 2))

    query_f = heads_of(queries)
    key_f = heads_of(cell_key_rows) * HEAD_DIM ** (-0.5)
    value_f = heads_of(cell_value_rows)
    forget_log_values = jax.nn.log_sigmoid(forget_gate_logits) + extra_log_forget
    running = jnp.cumsum(forget_log_values, axis=1)
    total_dev = running[:, -1]
    log_write = input_gate_logs + total_dev[:, None] - running
    stab_dev = jnp.max(log_write, axis=1)
    cell_dev = jnp.einsum(
        "hsd,hse->hde",
        key_f * jnp.exp(log_write - stab_dev[:, None])[..., None],
        value_f,
        precision=highest,
    )

    def weights_for(expert):
        return jnp.sum(jnp.where(routes == expert, token_expert_weights, 0.0), axis=1)

    def packed(expert):
        rows = [
            cell_dev.reshape(heads * HEAD_DIM, HEAD_DIM),
            jnp.broadcast_to(stab_dev[:, None], (heads, HEAD_DIM)),
            jnp.broadcast_to(total_dev[:, None], (heads, HEAD_DIM)),
            weights_for(expert).reshape(-1, HEAD_DIM),
        ]
        return jnp.concatenate(rows, axis=0)

    parts = [send(packed(sp_index ^ k), "sp", k) for k in (1, 2, 3)]
    cells, stabs, totals, dense = [], [], [], [weights_for(sp_index)]
    for part in parts:
        size = heads * HEAD_DIM
        cells.append(part[:size].reshape(heads, HEAD_DIM, HEAD_DIM))
        stabs.append(part[size : size + heads, 0])
        totals.append(part[size + heads : size + 2 * heads, 0])
        dense.append(part[size + 2 * heads :].reshape(-1))
    peers = [sp_index ^ k for k in (1, 2, 3)]
    prefix_total = sum(jnp.where(p < sp_index, total, 0.0) for p, total in zip(peers, totals))
    carried = []
    for p, stab in zip(peers, stabs):
        later = sum(
            jnp.where((q > p) & (q < sp_index), total, 0.0) for q, total in zip(peers, totals)
        )
        carried.append(jnp.where(p < sp_index, stab + later, floor_neg))
    start_stab = prefix_total
    for carry in carried:
        start_stab = jnp.maximum(start_stab, carry)
    start_cell = sum(
        jnp.exp(carry - start_stab)[:, None, None] * cell for carry, cell in zip(carried, cells)
    )
    numer = block_cells(
        query_f, key_f, value_f, input_gate_logs, forget_log_values, start_cell, start_stab
    )[0]
    scaled = (
        numer
        * lax.rsqrt(jnp.mean(numer * numer, axis=2, keepdims=True) + norm_eps)
        * head_norm_gain.reshape(heads, 1, HEAD_DIM)
    )
    mixed = jnp.transpose(scaled, (1, 0, 2)).reshape(length, heads * HEAD_DIM)
    cell_out = (jax.nn.sigmoid(output_gate_logits.astype(jnp.float32)) * mixed).astype(bf16)

    def by_place(x, axis):
        shape = x.shape[:axis] + (chips, 2, tokens) + x.shape[axis + 1 :]
        x = relative(x.reshape(shape), axis, chip)
        first, second = (lax.index_in_dim(x, i, axis + 1, keepdims=False) for i in (0, 1))
        return (jnp.where(core == 0, first, second), jnp.where(core == 0, second, first))

    cell_mine, cell_theirs = (
        part.reshape(chips * tokens, heads * HEAD_DIM) for part in by_place(cell_out, 0)
    )

    def project(rows):
        return jnp.dot(rows, cell_output_matrix, preferred_element_type=jnp.float32)

    from_core = send(project(cell_theirs).astype(bf16), "core")
    summed = (project(cell_mine) + from_core.astype(jnp.float32)).astype(bf16)
    summed = summed.reshape(chips, tokens, model)
    after = lax.dynamic_slice_in_dim(residual, tp_index * tokens, tokens, 0).astype(jnp.float32)
    after = after + summed[0].astype(jnp.float32)
    for j in order_of(chips)[1:]:
        after = after + send(summed[j], "chip", j).astype(jnp.float32)
    after_mix = after.astype(bf16)
    moe_in = rms_scale(after_mix, expert_norm_gain)

    weights_mine, weights_theirs = by_place(jnp.stack(dense), 1)
    gate_local, up_local, down_local = (
        expert_gate_matrix[0],
        expert_up_matrix[0],
        expert_down_matrix[0],
    )
    blocks = {0: moe_in}
    for j in order_of(chips)[1:]:
        blocks[j] = send(moe_in, "chip", -j)
    moe = None
    for j in order_of(chips):
        block = blocks[j]
        block_x, block_y = send(block, "sp", 1), send(block, "sp", 2)
        block_d = (send(block_x[:half], "sp", 2), send(block_y[half:], "sp", 1))
        mine = jnp.concatenate([block, block_x, block_y, *block_d], axis=0)
        rows = jnp.concatenate([mine, send(mine, "core")], axis=0)
        row_weights = jnp.concatenate(
            [weights_mine[:, j].reshape(-1), weights_theirs[:, j].reshape(-1)]
        )
        gate = jnp.dot(rows, gate_local, preferred_element_type=jnp.float32)
        upper = jnp.dot(rows, up_local, preferred_element_type=jnp.float32)
        hidden = (jax.nn.silu(gate) * upper * row_weights[:, None]).astype(bf16)
        count = 4 * tokens
        theirs = jnp.dot(hidden[count:], down_local, preferred_element_type=jnp.float32)
        ours = jnp.dot(hidden[:count], down_local, preferred_element_type=jnp.float32)
        ours = (ours + send(theirs.astype(bf16), "core").astype(jnp.float32)).astype(bf16)
        own, to_x, to_y, to_d = (ours[i * tokens : (i + 1) * tokens] for i in range(4))
        via_y, via_x = send(to_d[:half], "sp", 2), send(to_d[half:], "sp", 1)
        to_x = jnp.concatenate([to_x[:half] + via_y, to_x[half:]], axis=0)
        to_y = jnp.concatenate([to_y[:half], to_y[half:] + via_x], axis=0)
        own = (
            own.astype(jnp.float32)
            + send(to_x, "sp", 1).astype(jnp.float32)
            + send(to_y, "sp", 2).astype(jnp.float32)
        )
        if j:
            own = send(own.astype(bf16), "chip", j).astype(jnp.float32)
        moe = own if moe is None else moe + own
    return (after_mix.astype(jnp.float32) + moe).astype(bf16)


def order_of(chips):
    return sorted(range(chips), key=lambda j: min(j, chips - j))


def fits_dense(mesh):
    return mesh.shape["sp"] == 4 and mesh.shape["tp"] % 2 == 0


def solution(mesh):
    placed = (
        P("sp", "tp"),
        P("sp", "tp"),
        P("sp", "tp"),
        P("sp", "tp"),
        P("tp", "sp"),
        P("tp", "sp"),
        P("tp", "sp"),
        P("tp"),
        P("tp", None),
        P("sp", None),
        P(),
        P("sp", None),
        P("sp", None),
        P("sp", None, "tp"),
        P("sp", None, "tp"),
        P("sp", "tp", None),
    )
    body = dense_local if fits_dense(mesh) else local
    return jax.shard_map(
        body, mesh=mesh, in_specs=placed, out_specs=P(("sp", "tp"), None), check_vma=False
    )
```
